32 devices in a mesh: sp: 8 (over z, y), tp: 4 (over x, core).
Axes of the slice: x: 2, y: 2, z: 4, core: 2. Of those that a mesh axis runs over, the one named last changes fastest.
Arguments:
- resid: bfloat16 [4096, 2048], P('sp', 'tp'), may hold values from -41 to 41
- queries: bfloat16 [4096, 1024], P('sp', 'tp'), may hold values from -6 to 6
- keys: bfloat16 [4096, 1024], P('sp', 'tp'), may hold values from -6 to 6
- values: bfloat16 [4096, 1024], P('sp', 'tp'), may hold values from -6 to 6
- mix_lambda: float32 [8], P('tp'), may hold values from 0.3 to 0.8
- head_gain: float32 [128], replicated, may hold values from 0.1 to 1.9
- out_weight: bfloat16 [1024, 2048], P(None, 'tp'), may hold values from -0.1875 to 0.1875
- norm_gain: float32 [2048], P('tp'), may hold values from 0.1 to 1.9
- gate_weight: bfloat16 [2048, 5632], P('sp', 'tp'), may hold values from -0.125 to 0.125
- up_weight: bfloat16 [2048, 5632], P('sp', 'tp'), may hold values from -0.125 to 0.125
- conv_weight: float32 [3, 5632], P(None, 'tp'), may hold values from -3.5 to 3.5
- conv_bias: float32 [5632], P('tp'), may hold values from -3 to 3
- down_weight: bfloat16 [5632, 2048], P('tp', 'sp'), may hold values from -0.078125 to 0.078125
Outputs:
- layer_out: bfloat16 [4096, 2048], P('sp', 'tp')
The draws below stay inside these ranges and needn't reach their ends.
All inputs are finite; a program needn't handle non-finite values.
Results may differ from the reference program's by a relative error of at most 0.009.
Values may be sent and summed in bfloat16 or wider, within the bound.
No kernel may reach another device: no remote copies, remote signals or barrier semaphores. Data moves between devices by JAX's collectives and lax.ppermute only.
A program may use at most 128 MiB of HBM per device.

```python
import math
import jax
import jax.numpy as jnp
from jax import lax

D = 2048
HEADS = 8
HD = 64
VD = 128
FF = 5632
TOKENS = 4096
N_TP = 4


def pair_draw(key):
    width = HEADS * 2 * HD
    query_part = 1.3 * jnp.clip(jax.random.normal(jax.random.fold_in(key, 11), (TOKENS, width), jnp.float32), -4.0, 4.0)
    key_part = 1.3 * jnp.clip(jax.random.normal(jax.random.fold_in(key, 12), (TOKENS, width), jnp.float32), -4.0, 4.0)
    return (query_part, key_part)


def draw_queries(key, part):
    return pair_draw(key)[0].astype(jnp.bfloat16)


def draw_keys(key, part):
    return pair_draw(key)[1].astype(jnp.bfloat16)


def draw_resid(key, part):
    base = jax.random.fold_in(key, 21)
    row_scale = 10.0 ** (jax.random.uniform(jax.random.fold_in(base, 1), (TOKENS, 1), jnp.float32) - 0.5)
    position = jnp.arange(D, dtype=jnp.float32)[None, :] / D
    column_scale = 10.0 ** (0.7 * position + 0.3 * jax.random.uniform(jax.random.fold_in(base, 2), (1, D), jnp.float32) - 0.5)
    noise = jnp.clip(jax.random.normal(jax.random.fold_in(base, 4), (TOKENS, D), jnp.float32), -4.0, 4.0)
    return (noise * row_scale * column_scale).astype(jnp.bfloat16)


def levels(own_key, extent, pieces, smallest, high):
    loudness = 1.0
    for dim, blocks in pieces:
        steps = jax.random.uniform(jax.random.fold_in(jax.random.fold_in(own_key, 6), dim), (blocks,), jnp.float32, smallest / len(pieces), high / len(pieces))
        loudness = loudness * jnp.repeat(jnp.exp(steps), extent[dim] // blocks).reshape((-1,) + (1,) * (len(extent) - 1 - dim))
    return loudness


def normal_values(own_key, extent, scale, most, cuts=(), kind=jnp.bfloat16):
    level = levels(own_key, extent, cuts, -0.22, 0.18) if cuts else 1.0
    result = jax.random.normal(own_key, extent, jnp.float32) * scale * level
    return jnp.minimum(jnp.maximum(result, -most), most).astype(kind)


def setup_inputs(seed: int = 0) -> dict:
    arg_keys = jax.random.split(jax.random.key(seed), 14)
    resid = draw_resid(jax.random.fold_in(arg_keys[13], 71), 0)
    queries = draw_queries(jax.random.fold_in(arg_keys[13], 71), 0)
    keys = draw_keys(jax.random.fold_in(arg_keys[13], 71), 0)
    values = normal_values(arg_keys[3], (TOKENS, HEADS * VD), 1.0, 6.0, ((0, 8), (1, 4)))
    mix_lambda = jnp.clip(0.3 + 0.5 * jax.random.uniform(arg_keys[4], (HEADS,), jnp.float32) ** levels(arg_keys[4], (HEADS,), ((0, 4),), -0.2, 0.2), 0.3, 0.8)
    head_gain = jnp.clip(1.0 + 0.18 * jax.random.normal(arg_keys[5], (VD,), jnp.float32), 0.1, 1.9)
    out_weight = normal_values(arg_keys[6], (HEADS * VD, D), (HEADS * VD) ** -0.5, 0.1875, ((1, 4),))
    norm_gain = jnp.clip(1.0 + 0.18 * jax.random.normal(arg_keys[7], (D,), jnp.float32), 0.1, 1.9)
    gate_weight = normal_values(arg_keys[8], (D, FF), D ** -0.5, 0.125, ((0, 8), (1, 4)))
    up_weight = normal_values(arg_keys[9], (D, FF), D ** -0.5, 0.125, ((0, 8), (1, 4)))
    conv_weight = normal_values(arg_keys[10], (3, FF), 3 ** -0.5, 3.5, ((1, 4),), jnp.float32)
    conv_bias = normal_values(arg_keys[11], (FF,), 0.5, 3.0, ((0, 4),), jnp.float32)
    down_weight = normal_values(arg_keys[12], (FF, D), FF ** -0.5, 0.078125, ((0, 4), (1, 8)))
    return {"resid": resid, "queries": queries, "keys": keys, "values": values, "mix_lambda": mix_lambda, "head_gain": head_gain, "out_weight": out_weight, "norm_gain": norm_gain, "gate_weight": gate_weight, "up_weight": up_weight, "conv_weight": conv_weight, "conv_bias": conv_bias, "down_weight": down_weight}


def head_attention(query_head, key_head, value_head, weight_two):
    length = query_head.shape[0]
    scale = HD ** (-0.5)
    block = math.gcd(length, 512)
    query_blocks = query_head.reshape(length // block, block, 2, HD)
    key_float = key_head.astype(jnp.float32)
    value_float = value_head.astype(jnp.float32)

    def one_block(query_block):
        scores = jnp.einsum('qmd,kmd->mqk', query_block.astype(jnp.float32), key_float) * scale
        highest = lax.optimization_barrier(jnp.max(scores, axis=-1, keepdims=True))
        shifted = jnp.exp(scores - highest)
        totals = lax.optimization_barrier(jnp.sum(shifted, axis=-1))
        unnormed = lax.optimization_barrier(shifted.astype(jnp.bfloat16)).astype(jnp.float32)
        mapped = jnp.einsum('mqk,ke->mqe', unnormed, value_float) / totals[..., None]
        return mapped[0] - weight_two * mapped[1]
    return lax.map(one_block, query_blocks).reshape(length, VD)

def reference(resid, queries, keys, values, mix_lambda, head_gain, out_weight, norm_gain, gate_weight, up_weight, conv_weight, conv_bias, down_weight):
    length = queries.shape[0]
    query_heads = jnp.transpose(queries.reshape(length, HEADS, 2, HD), (1, 0, 2, 3))
    key_heads = jnp.transpose(keys.reshape(length, HEADS, 2, HD), (1, 0, 2, 3))
    value_heads = jnp.transpose(values.reshape(length, HEADS, VD), (1, 0, 2))
    mixed = lax.map(lambda parts: head_attention(parts[0], parts[1], parts[2], parts[3]), (query_heads, key_heads, value_heads, mix_lambda))
    spread = lax.optimization_barrier(jnp.mean(mixed * mixed, axis=-1, keepdims=True))
    normed = mixed * lax.rsqrt(spread + 1e-06) * head_gain * 0.8
    heads_out = jnp.transpose(normed, (1, 0, 2)).reshape(length, HEADS * VD).astype(jnp.bfloat16)
    after_mixer = resid.astype(jnp.float32) + jnp.dot(heads_out, out_weight, preferred_element_type=jnp.float32)
    squares = lax.optimization_barrier(jnp.mean(after_mixer * after_mixer, axis=-1, keepdims=True))
    normed_rows = (after_mixer * lax.rsqrt(squares + 1e-06) * norm_gain).astype(jnp.bfloat16)
    gated = jnp.dot(normed_rows, gate_weight, preferred_element_type=jnp.float32).astype(jnp.bfloat16)
    upward = jnp.dot(normed_rows, up_weight, preferred_element_type=jnp.float32)
    padded = jnp.pad(gated.astype(jnp.float32), ((1, 1), (0, 0)))
    conv = padded[:-2] * conv_weight[0] + padded[1:-1] * conv_weight[1] + padded[2:] * conv_weight[2] + conv_bias
    hidden = (jax.nn.silu(conv) * upward).astype(jnp.bfloat16)
    span = FF // N_TP
    hidden_blocks = jnp.transpose(hidden.reshape(length, N_TP, span), (1, 0, 2))
    down_blocks = down_weight.reshape(N_TP, span, D)

    def block_sum(carry, pair):
        part = jnp.dot(pair[0], pair[1], preferred_element_type=jnp.float32).astype(jnp.bfloat16)
        return (carry + part.astype(jnp.float32), None)
    mixer_out, unused = lax.scan(block_sum, jnp.zeros((length, D), jnp.float32), (hidden_blocks, down_blocks))
    return (after_mixer + mixer_out).astype(jnp.bfloat16)
```

```python
import functools

import jax
import jax.numpy as jnp
from jax import lax
from jax.experimental import pallas as pl
from jax.experimental.pallas import tpu as pltpu
from jax.sharding import PartitionSpec as P

HD = 64
VD = 128
PAD = 16


def attend_kernel(heads, chunks, first, last, *refs):
    q_ref = refs[0]
    k_refs = refs[1 : 1 + chunks]
    v_refs = refs[1 + chunks : 1 + 2 * chunks]
    rest = refs[1 + 2 * chunks :]
    if not first:
        m_in, a_in = rest[:2]
        rest = rest[2:]
    if last:
        lam_ref, gain_ref, out_ref = rest
    else:
        m_out, a_out = rest
    rows = q_ref.shape[0]
    lane = lax.broadcasted_iota(jnp.int32, (rows, 2 * HD), 1)
    for h in range(heads):
        cols = slice(h * 2 * HD, (h + 1) * 2 * HD)
        q_head = q_ref[:, cols]
        k_head = [k[:, cols] for k in k_refs]
        v_head = [
            jnp.concatenate(
                [v[:, h * VD : (h + 1) * VD], jnp.ones((v.shape[0], VD), v.dtype)], axis=1
            )
            for v in v_refs
        ]
        mapped = []
        for i in range(2):
            keep = (lane < HD) if i == 0 else (lane >= HD)
            q_map = jnp.where(keep, q_head, jnp.zeros_like(q_head))
            scores = [
                lax.dot_general(
                    q_map, k, (((1,), (1,)), ((), ())), preferred_element_type=jnp.float32
                )
                for k in k_head
            ]
            high = functools.reduce(
                jnp.maximum, [jnp.max(s, axis=1, keepdims=True) for s in scores]
            )
            if not first:
                before = m_in[h, i][:, :1]
                high = jnp.maximum(before, high)
            total = None
            for s, v in zip(scores, v_head):
                part = jnp.dot(
                    jnp.exp(s - high).astype(jnp.bfloat16), v, preferred_element_type=jnp.float32
                )
                total = part if total is None else total + part
            if not first:
                total = total + a_in[h, i] * jnp.exp(before - high)
            if last:
                mapped.append(total[:, :VD] / total[:, VD:])
            else:
                m_out[h, i] = jnp.broadcast_to(high, (rows, 128))
                a_out[h, i] = total
        if last:
            mixed = mapped[0] - lam_ref[h] * mapped[1]
            spread = jnp.mean(mixed * mixed, axis=1, keepdims=True)
            normed = mixed * lax.rsqrt(spread + 1e-06) * gain_ref[...] * 0.8
            out_ref[:, h * VD : (h + 1) * VD] = normed.astype(out_ref.dtype)


def attend(q, ks, vs, carry, final, heads):
    rows = q.shape[0]
    count = sum(k.shape[0] for k in ks)
    vmem = pl.BlockSpec(memory_space=pltpu.VMEM)
    args = [q, *ks, *vs]
    specs = [vmem] * len(args)
    if carry is not None:
        args += list(carry)
        specs += [vmem] * 2
    if final is not None:
        args += list(final)
        specs += [pl.BlockSpec(memory_space=pltpu.SMEM), vmem]
        out = jax.ShapeDtypeStruct((rows, heads * VD), jnp.bfloat16)
        out_specs = vmem
    else:
        out = [
            jax.ShapeDtypeStruct((heads, 2, rows, 128), jnp.float32),
            jax.ShapeDtypeStruct((heads, 2, rows, 2 * VD), jnp.float32),
        ]
        out_specs = [vmem] * 2
    work = rows * count * heads * 2
    return pl.pallas_call(
        functools.partial(attend_kernel, heads, len(ks), carry is None, final is not None),
        out_shape=out,
        in_specs=specs,
        out_specs=out_specs,
        compiler_params=pltpu.CompilerParams(vmem_limit_bytes=56 * 1024 * 1024),
        cost_estimate=pl.CostEstimate(
            flops=work * 1200, bytes_accessed=4 * 1024 * 1024, transcendentals=work
        ),
    )(*args)


def after(value, *others):
    return lax.optimization_barrier((value, *others))[0]


def ring_order(count):
    if count % 2:
        return list(range(count))
    return list(range(0, count, 2)) + list(range(count - 1, 0, -2))


class Ring:
    def __init__(self, axis, own, axis_cut=0):
        self.axis = axis
        self.count = lax.axis_size(axis)
        order = ring_order(self.count)
        n = self.count
        self.ahead = [(order[i], order[(i + 1) % n]) for i in range(n)]
        self.back = [(order[(i + 1) % n], order[i]) for i in range(n)]
        self.own = own
        self.cut = axis_cut
        place = [0] * n
        for i, o in enumerate(order):
            place[o] = i
        self.order = jnp.array(order, jnp.int32)
        self.place = jnp.array(place, jnp.int32)[lax.axis_index(axis)]
        self.a = own
        self.b = own
        self.step_no = 0
        self.steps = (n - 1 + 1) // 2

    def at(self, shift):
        return self.order[(self.place + shift) % self.count]

    def step(self, *behind):
        self.step_no += 1
        s = self.step_no
        a, b = self.a, self.b
        if behind:
            a, b = lax.optimization_barrier((a, b, *behind))[:2]
        if self.count % 2 == 0 and s == self.steps:
            half = self.own.shape[self.cut] // 2
            low = lax.slice_in_dim(a, 0, half, axis=self.cut)
            high = lax.slice_in_dim(b, half, 2 * half, axis=self.cut)
            low = lax.ppermute(low, self.axis, self.ahead)
            high = lax.ppermute(high, self.axis, self.back)
            return [((low, high), self.at(s))]
        self.a = lax.ppermute(a, self.axis, self.ahead)
        self.b = lax.ppermute(b, self.axis, self.back)
        return [(self.a, self.at(-s)), (self.b, self.at(s))]


def tails(blocks):
    out = []
    for block, where in blocks:
        out += list(block) if isinstance(block, tuple) else [block]
    return out


def on_device(
    resid,
    queries,
    keys,
    values,
    mix_lambda,
    head_gain,
    out_weight,
    norm_gain,
    gate_weight,
    up_weight,
    conv_weight,
    conv_bias,
    down_weight,
):
    length = queries.shape[0]
    heads = mix_lambda.shape[0]
    n_sp = lax.axis_size("sp")
    n_tp = lax.axis_size("tp")
    sp = lax.axis_index("sp")
    tp = lax.axis_index("tp")
    width = resid.shape[1] * n_tp
    onward = [(i, i + 1) for i in range(n_sp - 1)]
    backward = [(i + 1, i) for i in range(n_sp - 1)]

    def extended(x, fill):
        before = lax.ppermute(x[-1:], "sp", onward)
        behind = lax.ppermute(x[:1], "sp", backward)
        spare = jnp.zeros((fill - 2, x.shape[1]), x.dtype)
        return jnp.concatenate([x, before, behind, spare], axis=0)

    q = extended(queries * jnp.asarray(HD**-0.5, queries.dtype), PAD)
    resid_ext = extended(resid, PAD)
    out_full = lax.all_gather(out_weight, "tp", axis=1, tiled=True)
    resid_full = lax.all_gather(resid_ext, "tp", axis=1, tiled=True)
    gain_full = lax.all_gather(norm_gain, "tp", axis=0, tiled=True)

    k_ring = Ring("sp", keys)
    v_ring = Ring("sp", values)
    gate_ring = Ring("sp", gate_weight)
    up_ring = Ring("sp", up_weight)
    down_ring = Ring("sp", down_weight)
    steps = k_ring.steps

    final = (mix_lambda, head_gain.reshape(1, VD))
    carry = attend(q, [keys], [values], None, None, heads)
    held = None
    for s in range(steps):
        if s + 1 == steps:
            held = tails(new_k) + tails(new_v)
        new_k = k_ring.step()
        new_v = v_ring.step()
        carry = attend(
            q,
            tails(new_k),
            tails(new_v),
            carry,
            final if s + 1 == steps else None,
            heads,
        )
    mine = carry

    gate_blocks = [(gate_weight, sp)]
    up_blocks = [(up_weight, sp)]
    down_blocks = [(down_weight, sp)]
    for s in range(steps):
        extra = held if s == 0 else []
        if s + 1 == steps:
            held = tails(gate_blocks[-2:]) + tails(up_blocks[-2:])
        gate_blocks += gate_ring.step(*extra)
        up_blocks += up_ring.step(*extra)
    for s in range(steps):
        down_blocks += down_ring.step(*(held if s == 0 else []))

    pieces = [(mine, 0)]
    bit = n_tp // 2
    while bit:
        pairs = [(i, i ^ bit) for i in range(n_tp)]
        pieces += [(lax.ppermute(p, "tp", pairs), mask ^ bit) for p, mask in pieces]
        bit //= 2
    span = heads * VD
    projected = resid_full.astype(jnp.float32)
    for piece, mask in pieces:
        rows = lax.dynamic_slice_in_dim(out_full, (tp ^ mask) * span, span, axis=0)
        projected = projected + jnp.dot(piece, rows, preferred_element_type=jnp.float32)
    after_mixer = projected
    squares = jnp.mean(after_mixer * after_mixer, axis=1, keepdims=True)
    normed_rows = (after_mixer * lax.rsqrt(squares + 1e-06) * gain_full).astype(jnp.bfloat16)
    own_mixer = lax.dynamic_slice(
        after_mixer, (0, tp * resid.shape[1]), (length, resid.shape[1])
    )

    def rows_times(blocks, rows):
        total = None
        for block, where in blocks:
            parts = list(block) if isinstance(block, tuple) else [block]
            start = where * (width // n_sp)
            for part in parts:
                cols = lax.dynamic_slice_in_dim(rows, start, part.shape[0], axis=1)
                term = jnp.dot(cols, part, preferred_element_type=jnp.float32)
                total = term if total is None else total + term
                start = start + part.shape[0]
        return total

    gated = rows_times(gate_blocks, normed_rows).astype(jnp.bfloat16)
    upward = rows_times(up_blocks, normed_rows[:length])
    before = jnp.where(sp == 0, 0, gated[length : length + 1])
    behind = jnp.where(sp == n_sp - 1, 0, gated[length + 1 : length + 2])
    middle = gated[:length]
    conv = (
        jnp.concatenate([before, middle[:-1]], axis=0).astype(jnp.float32) * conv_weight[0]
        + middle.astype(jnp.float32) * conv_weight[1]
        + jnp.concatenate([middle[1:], behind], axis=0).astype(jnp.float32) * conv_weight[2]
        + conv_bias
    )
    hidden = (jax.nn.silu(conv) * upward).astype(jnp.bfloat16)

    slab = width // n_sp
    partial = jnp.zeros((n_sp, length, slab), jnp.bfloat16)
    for block, where in down_blocks:
        if isinstance(block, tuple):
            block = jnp.concatenate(block, axis=0)
        term = jnp.dot(hidden, block, preferred_element_type=jnp.float32).astype(jnp.bfloat16)
        partial = lax.dynamic_update_slice(partial, term[None], (where, 0, 0))
    partial = partial.reshape(n_tp, n_sp // n_tp, length, slab)
    bit = 1
    while bit < n_tp:
        groups = partial.reshape(partial.shape[0] // 2, 2, *partial.shape[1:])
        mine_bit = (tp // bit) % 2
        keep = lax.dynamic_index_in_dim(groups, mine_bit, axis=1, keepdims=False)
        give = lax.dynamic_index_in_dim(groups, 1 - mine_bit, axis=1, keepdims=False)
        pairs = [(i, i ^ bit) for i in range(n_tp)]
        got = lax.ppermute(give.astype(jnp.bfloat16), "tp", pairs)
        partial = keep.astype(jnp.float32) + got.astype(jnp.float32)
        bit *= 2
    summed = jnp.transpose(partial[0], (1, 0, 2)).reshape(length, -1)
    return (own_mixer + summed).astype(jnp.bfloat16)


def solution(mesh):
    placed = (
        P("sp", "tp"),
        P("sp", "tp"),
        P("sp", "tp"),
        P("sp", "tp"),
        P("tp"),
        P(),
        P(None, "tp"),
        P("tp"),
        P("sp", "tp"),
        P("sp", "tp"),
        P(None, "tp"),
        P("tp"),
        P("tp", "sp"),
    )
    return jax.shard_map(
        on_device, mesh=mesh, in_specs=placed, out_specs=P("sp", "tp"), check_vma=False
    )
```
